32 devices in a mesh: grp: 2 (over y), ra: 4 (over z), cb: 2 (over x), dp: 2 (over core).
Axes of the slice: x: 2, y: 2, z: 4, core: 2. Of those that a mesh axis runs over, the one named last changes fastest.
Arguments:
- tokens: bfloat16 [256, 2048], P(('grp', 'dp'), 'ra'), parts along dimension 0, may hold values from -51 to 51
- first_gain: float32 [2048], P('ra'), may hold values from 0.1 to 1.9
- first_gate: float32 [2048, 5632], P('ra', 'cb'), may hold values from -0.125 to 0.125
- first_up: float32 [2048, 5632], P('ra', 'cb'), may hold values from -0.125 to 0.125
- first_down: float32 [5632, 2048], P('cb', 'ra'), may hold values from -0.078125 to 0.078125
- first_gate_scale: float32 [5632], P('cb'), may hold values from 0.1 to 1.9
- first_up_scale: float32 [5632], P('cb'), may hold values from 0.1 to 1.9
- first_down_scale: float32 [2048], P('ra'), may hold values from 0.1 to 1.9
- second_gain: float32 [2048], P('ra'), may hold values from 0.1 to 1.9
- second_gate: float32 [2048, 5632], P('ra', 'cb'), may hold values from -0.125 to 0.125
- second_up: float32 [2048, 5632], P('ra', 'cb'), may hold values from -0.125 to 0.125
- second_down: float32 [5632, 2048], P('cb', 'ra'), may hold values from -0.078125 to 0.078125
- second_gate_scale: float32 [5632], P('cb'), may hold values from 0.1 to 1.9
- second_up_scale: float32 [5632], P('cb'), may hold values from 0.1 to 1.9
- second_down_scale: float32 [2048], P('ra'), may hold values from 0.1 to 1.9
Outputs:
- result: bfloat16 [256, 2048], P(('grp', 'dp'), 'ra'), parts along dimension 0
The draws below stay inside these ranges and needn't reach their ends.
There are 2 independent parts, one for each index of `grp`. The reference program is written for one: setup_inputs(seed, part) draws one part's arguments, and reference() takes and returns one part's arrays. A program takes and returns all parts, laid end to end along the dimension named above; an argument that names none is the same for every part. Nothing has to cross between parts.
All inputs are finite; a program needn't handle non-finite values.
Results may differ from the reference program's by a relative error of at most 0.04.
Values may be sent and summed in bfloat16 or wider, within the bound.
A program may use at most 64 MiB of HBM per device.

```python
import jax
import jax.numpy as jnp
from jax import lax

D = 2048
FF = 5632
TOKENS = 128
N_CB = 2


def draw_tokens(key, part):
    key_base = jax.random.fold_in(key, 11)
    key_rough = jax.random.fold_in(key, 12)
    columns = jnp.arange(D).astype(jnp.float32)
    rising = 3.0 ** (columns / D)
    rough = jnp.exp(jax.random.uniform(key_rough, (D,), jnp.float32, -0.35, 0.35))
    base = jnp.clip(jax.random.normal(key_base, (TOKENS, D), jnp.float32), -3.0, 3.0)
    return (base * rising * rough * 0.7).astype(jnp.bfloat16)


def steps_of(own_key, dims, shards, smallest, high):
    def one(position, parts):
        heights = jax.random.uniform(jax.random.fold_in(jax.random.fold_in(own_key, 6), position), (parts,), jnp.float32, smallest / len(shards), high / len(shards))
        return jnp.repeat(jnp.exp(heights), dims[position] // parts).reshape((-1,) + (1,) * (len(dims) - position - 1))

    factor_of = one(*shards[0])
    for cut in shards[1:]:
        factor_of = factor_of * one(*cut)
    return factor_of


def centred(stream_key, shape, scale, bound, pieces=(), dtype=jnp.bfloat16):
    result = scale * jax.random.normal(stream_key, shape, jnp.float32)
    if pieces:
        result = result * steps_of(stream_key, shape, pieces, -0.22, 0.18)
    return jnp.clip(result, -bound, bound).astype(dtype)


def setup_inputs(seed: int = 0, part: int = 0) -> dict:
    streams_of = jax.random.split(jax.random.key(seed), 16)
    own_keys = jax.random.split(jax.random.fold_in(streams_of[15], part), 16)
    tokens = draw_tokens(jax.random.fold_in(jax.random.fold_in(streams_of[15], part), 71), part)
    first_gain = jnp.clip(1.0 + 0.18 * jax.random.normal(streams_of[1], (D,), jnp.float32), 0.1, 1.9)
    first_gate = centred(streams_of[2], (D, FF), D ** -0.5, 0.125, ((0, 4), (1, 2)), jnp.float32)
    first_up = centred(streams_of[3], (D, FF), D ** -0.5, 0.125, ((0, 4), (1, 2)), jnp.float32)
    first_down = centred(streams_of[4], (FF, D), FF ** -0.5, 0.078125, ((0, 2), (1, 4)), jnp.float32)
    first_gate_scale = jnp.clip(1.0 + 0.18 * jax.random.normal(streams_of[5], (FF,), jnp.float32), 0.1, 1.9)
    first_up_scale = jnp.clip(1.0 + 0.18 * jax.random.normal(streams_of[6], (FF,), jnp.float32), 0.1, 1.9)
    first_down_scale = jnp.clip(1.0 + 0.18 * jax.random.normal(streams_of[7], (D,), jnp.float32), 0.1, 1.9)
    second_gain = jnp.clip(1.0 + 0.18 * jax.random.normal(streams_of[8], (D,), jnp.float32), 0.1, 1.9)
    second_gate = centred(streams_of[9], (D, FF), D ** -0.5, 0.125, ((0, 4), (1, 2)), jnp.float32)
    second_up = centred(streams_of[10], (D, FF), D ** -0.5, 0.125, ((0, 4), (1, 2)), jnp.float32)
    second_down = centred(streams_of[11], (FF, D), FF ** -0.5, 0.078125, ((0, 2), (1, 4)), jnp.float32)
    second_gate_scale = jnp.clip(1.0 + 0.18 * jax.random.normal(streams_of[12], (FF,), jnp.float32), 0.1, 1.9)
    second_up_scale = jnp.clip(1.0 + 0.18 * jax.random.normal(streams_of[13], (FF,), jnp.float32), 0.1, 1.9)
    second_down_scale = jnp.clip(1.0 + 0.18 * jax.random.normal(streams_of[14], (D,), jnp.float32), 0.1, 1.9)
    return dict(tokens=tokens, first_gain=first_gain, first_gate=first_gate, first_up=first_up, first_down=first_down, first_gate_scale=first_gate_scale, first_up_scale=first_up_scale, first_down_scale=first_down_scale, second_gain=second_gain, second_gate=second_gate, second_up=second_up, second_down=second_down, second_gate_scale=second_gate_scale, second_up_scale=second_up_scale, second_down_scale=second_down_scale)


EPS = 1e-06

def sublayer(values, gain, w_gate, w_up, w_down, gate_scale, up_scale, down_scale):
    floats = values.astype(jnp.float32)
    inverse = lax.rsqrt(lax.optimization_barrier(jnp.mean(floats * floats, axis=1, keepdims=True)) + EPS)
    scaled = (floats * gain).astype(jnp.bfloat16)
    gate = jnp.dot(scaled, w_gate.astype(jnp.bfloat16), preferred_element_type=jnp.float32) * gate_scale * inverse
    up_val = jnp.dot(scaled, w_up.astype(jnp.bfloat16), preferred_element_type=jnp.float32) * up_scale * inverse
    hidden = (jax.nn.silu(gate) * up_val).astype(jnp.bfloat16)
    block = FF // N_CB
    rows = hidden.shape[0]
    hidden_blocks = hidden.reshape(rows, N_CB, block).astype(jnp.float32)
    down_blocks = w_down.astype(jnp.bfloat16).reshape(N_CB, block, D).astype(jnp.float32)
    partial_terms = jnp.einsum('tcf,cfd->ctd', hidden_blocks, down_blocks).astype(jnp.bfloat16)
    partial_terms = lax.optimization_barrier(partial_terms)
    down = lax.optimization_barrier(jnp.sum(partial_terms.astype(jnp.float32), axis=0))
    return (0.3 * floats + 0.5 * down * down_scale).astype(jnp.bfloat16)

def reference(tokens, first_gain, first_gate, first_up, first_down, first_gate_scale, first_up_scale, first_down_scale, second_gain, second_gate, second_up, second_down, second_gate_scale, second_up_scale, second_down_scale):
    middle = sublayer(tokens, first_gain, first_gate, first_up, first_down, first_gate_scale, first_up_scale, first_down_scale)
    return sublayer(middle, second_gain, second_gate, second_up, second_down, second_gate_scale, second_up_scale, second_down_scale)
```

```python
import functools

import jax
import jax.numpy as jnp
from jax import lax
from jax.experimental import pallas as pl
from jax.experimental.pallas import tpu as pltpu
from jax.sharding import PartitionSpec as P

EPS = 1e-06
MESH = pl.DeviceIdType.MESH
LANES = 128
LAG_SUM = 3
LAG_HID = 3


def kernel(dims, *refs):
    n, m, rows, width, units, total_width = dims
    (tokens, gain0, gate0, up0, down0, gs0, us0, ds0, gain1, gate1, up1, down1, gs1, us1, ds1) = refs[:15]
    out = refs[15]
    (values, scaled, gains, dscales, gscales, uscales, w_gu, w_down, own, sum_out, sum_in, hid, acc,
     down_in, squares, inverse, small_sem, gate_sem, up_sem, down_sem, sum_ss, sum_rs, hid_ss, hid_rs,
     part_ss, part_rs, sq_ss, sq_rs) = refs[16:]
    gate, up, down = (gate0, gate1), (up0, up1), (down0, down1)
    bf16, f32 = jnp.bfloat16, jnp.float32

    z, x = lax.axis_index("ra"), lax.axis_index("cb")
    blocks = units // LANES
    counts = (blocks - blocks // 2, blocks // 2)
    starts = (0, counts[0])
    place = (n - 1 - z, z)
    step = (-1, 1)
    pairs = counts[0]
    slots = max(2 * pairs, pairs + LAG_SUM * (n - 1) + LAG_HID * (n - 1))

    def copy_small():
        found = []
        for i, (src, dst) in enumerate((
            (tokens, values), (gain0, gains.at[0]), (gs0, gscales.at[0]), (us0, uscales.at[0]), (ds0, dscales.at[0]),
            (gain1, gains.at[1]), (gs1, gscales.at[1]), (us1, uscales.at[1]), (ds1, dscales.at[1]),
        )):
            found.append(pltpu.make_async_copy(src, dst, small_sem.at[i]))
        return found

    def columns(c):
        return pl.ds(pl.multiple_of(c * LANES, LANES), LANES)

    def gate_copy(l, c):
        return pltpu.make_async_copy(gate[l].at[:, columns(c)], w_gu.at[l, c, :, pl.ds(0, LANES)], gate_sem.at[l, c])

    def up_copy(l, c):
        return pltpu.make_async_copy(up[l].at[:, columns(c)], w_gu.at[l, c, :, pl.ds(LANES, LANES)], up_sem.at[l, c])

    def down_copy(l, c):
        return pltpu.make_async_copy(down[l].at[columns(c), :], w_down.at[l, c], down_sem.at[l, c])

    def sum_copy(l, c, d):
        return pltpu.make_async_remote_copy(
            src_ref=sum_out.at[l, c], dst_ref=sum_in.at[l, c], send_sem=sum_ss.at[l, c], recv_sem=sum_rs.at[l, c],
            device_id={"ra": z + step[d]}, device_id_type=MESH)

    def hid_copy(l, c, d):
        return pltpu.make_async_remote_copy(
            src_ref=hid.at[l, c], dst_ref=hid.at[l, c], send_sem=hid_ss.at[l, c], recv_sem=hid_rs.at[l, c],
            device_id={"ra": z - step[d]}, device_id_type=MESH)

    def part_copy(l, o, sender):
        return pltpu.make_async_remote_copy(
            src_ref=down_in.at[l, sender], dst_ref=down_in.at[l, sender], send_sem=part_ss.at[l, o],
            recv_sem=part_rs.at[l, sender], device_id={"cb": lax.rem(x + o, m)}, device_id_type=MESH)

    def sq_copy(l, end, sender):
        return pltpu.make_async_remote_copy(
            src_ref=squares.at[l, sender], dst_ref=squares.at[l, sender], send_sem=sq_ss.at[l, end],
            recv_sem=sq_rs.at[l, sender], device_id={"ra": end * (n - 1)}, device_id_type=MESH)

    def each_pair(i, act):
        for d in range(2):
            if counts[0] == counts[1]:
                act(starts[d] + i)
            else:
                @pl.when(i < counts[d])
                def _():
                    act(starts[d] + i)

    small = copy_small()
    for copy in small:
        copy.start()

    def start_first(i, carry):
        def act(c):
            gate_copy(0, c).start()
            up_copy(0, c).start()
        each_pair(i, act)
        return carry

    lax.fori_loop(0, pairs, start_first, 0)

    barrier = pltpu.get_barrier_semaphore()
    for o in range(1, n):
        pl.semaphore_signal(barrier, inc=1, device_id={"ra": lax.rem(z + o, n)}, device_id_type=MESH)
    for o in range(1, m):
        pl.semaphore_signal(barrier, inc=1, device_id={"cb": lax.rem(x + o, m)}, device_id_type=MESH)
    for copy in small:
        copy.wait()

    for l in range(2):
        floats = values[...].astype(f32)
        scaled[...] = (floats * gains[l]).astype(bf16)
        squares[l, z] = lax.dot_general(
            jnp.ones((8, width), f32), floats * floats, (((1,), (1,)), ((), ())),
            precision=lax.Precision.HIGHEST, preferred_element_type=f32)
        acc[...] = jnp.zeros_like(acc)
        if l == 0:
            pl.semaphore_wait(barrier, n + m - 2)
        for end in range(2):
            @pl.when(z != end * (n - 1))
            def _():
                sq_copy(l, end, z).start()

        def use_hidden(c, block):
            down_copy(l, c).wait()
            acc[...] += jnp.dot(block, w_down[l, c].astype(bf16), preferred_element_type=f32)

        def slot(s, carry):
            if l == 0:
                @pl.when(s < pairs)
                def _():
                    each_pair(s, lambda c: down_copy(0, c).start())

                @pl.when((s >= pairs) & (s < 2 * pairs))
                def _():
                    def act(c):
                        gate_copy(1, c).start()
                        up_copy(1, c).start()
                        down_copy(1, c).start()
                    each_pair(s - pairs, act)

            @pl.when(s < pairs)
            def _():
                def act(c):
                    gate_copy(l, c).wait()
                    up_copy(l, c).wait()
                    own[c] = jnp.dot(scaled[...], w_gu[l, c].astype(bf16), preferred_element_type=f32)
                each_pair(s, act)

            for d in range(2):
                p = place[d]
                k = s - LAG_SUM * p
                c = starts[d] + k
                turn = (k >= 0) & (k < counts[d])

                @pl.when(turn & (p == 0))
                def _():
                    sum_out[l, c] = own[c].astype(bf16)
                    sum_copy(l, c, d).start()

                @pl.when(turn & (p > 0) & (p < n - 1))
                def _():
                    sum_copy(l, c, d).wait_recv()
                    sum_out[l, c] = (own[c] + sum_in[l, c].astype(f32)).astype(bf16)
                    sum_copy(l, c, d).start()

                @pl.when(turn & (p == n - 1))
                def _():
                    @pl.when(k == 0)
                    def _():
                        for o in range(1, n):
                            sq_copy(l, 0, lax.rem(z + o, n)).wait_recv()
                        every = squares[l].reshape(8 * n, rows)
                        total = lax.dot_general(
                            every, jnp.full((8 * n, LANES), 0.125, f32), (((0,), (0,)), ((), ())),
                            precision=lax.Precision.HIGHEST, preferred_element_type=f32)
                        inverse[...] = lax.rsqrt(total / total_width + EPS)

                    sum_copy(l, c, d).wait_recv()
                    both = own[c] + sum_in[l, c].astype(f32)
                    inv = inverse[...]
                    g = both[:, :LANES] * gscales[l, :, columns(c)] * inv
                    u = both[:, LANES:] * uscales[l, :, columns(c)] * inv
                    block = (g / (1.0 + jnp.exp(-g)) * u).astype(bf16)
                    hid[l, c] = block
                    hid_copy(l, c, d).start()
                    use_hidden(c, block)

                k2 = s - LAG_SUM * (n - 1) - LAG_HID * (n - 1 - p)
                c2 = starts[d] + k2

                @pl.when((k2 >= 0) & (k2 < counts[d]) & (p < n - 1))
                def _():
                    hid_copy(l, c2, d).wait_recv()

                    @pl.when(p > 0)
                    def _():
                        hid_copy(l, c2, d).start()

                    use_hidden(c2, hid[l, c2])
            return carry

        lax.fori_loop(0, slots, slot, 0)

        down_in[l, x] = acc[...].astype(bf16)
        for o in range(1, m):
            part_copy(l, o, x).start()
        for o in range(1, m):
            part_copy(l, o, lax.rem(x + o, m)).wait_recv()
        total = down_in[l, 0].astype(f32)
        for o in range(1, m):
            total = total + down_in[l, o].astype(f32)
        result = (0.3 * values[...].astype(f32) + 0.5 * total * dscales[l]).astype(bf16)
        if l == 0:
            values[...] = result
        else:
            out[...] = result

    for l in range(2):
        for o in range(1, m):
            part_copy(l, o, x).wait_send()
        for end in range(2):
            @pl.when(z != end * (n - 1))
            def _():
                sq_copy(l, end, z).wait_send()
        for d in range(2):
            p = place[d]

            @pl.when(p < n - 1)
            def _():
                def body(k, carry):
                    sum_copy(l, starts[d] + k, d).wait_send()
                    return carry
                lax.fori_loop(0, counts[d], body, 0)

            @pl.when(p > 0)
            def _():
                def body(k, carry):
                    hid_copy(l, starts[d] + k, d).wait_send()
                    return carry
                lax.fori_loop(0, counts[d], body, 0)


def per_device(n, m, *args):
    tokens = args[0]
    rows, width = tokens.shape
    units = args[2].shape[1]
    blocks = units // LANES
    bf16, f32 = jnp.bfloat16, jnp.float32
    flat = [a.reshape(1, -1) if a.ndim == 1 else a for a in args]
    dma = pltpu.SemaphoreType.DMA
    return pl.pallas_call(
        functools.partial(kernel, (n, m, rows, width, units, n * width)),
        out_shape=jax.ShapeDtypeStruct((rows, width), bf16),
        in_specs=[pl.BlockSpec(memory_space=pl.ANY)] * len(flat),
        out_specs=pl.BlockSpec(memory_space=pltpu.VMEM),
        scratch_shapes=[
            pltpu.VMEM((rows, width), bf16),
            pltpu.VMEM((rows, width), bf16),
            pltpu.VMEM((2, 1, width), f32),
            pltpu.VMEM((2, 1, width), f32),
            pltpu.VMEM((2, 1, units), f32),
            pltpu.VMEM((2, 1, units), f32),
            pltpu.VMEM((2, blocks, width, 2 * LANES), f32),
            pltpu.VMEM((2, blocks, LANES, width), f32),
            pltpu.VMEM((blocks, rows, 2 * LANES), f32),
            pltpu.VMEM((2, blocks, rows, 2 * LANES), bf16),
            pltpu.VMEM((2, blocks, rows, 2 * LANES), bf16),
            pltpu.VMEM((2, blocks, rows, LANES), bf16),
            pltpu.VMEM((rows, width), f32),
            pltpu.VMEM((2, m, rows, width), bf16),
            pltpu.VMEM((2, n, 8, rows), f32),
            pltpu.VMEM((rows, LANES), f32),
            dma((9,)),
            dma((2, blocks)),
            dma((2, blocks)),
            dma((2, blocks)),
            dma((2, blocks)),
            dma((2, blocks)),
            dma((2, blocks)),
            dma((2, blocks)),
            dma((2, m)),
            dma((2, m)),
            dma((2, 2)),
            dma((2, n)),
        ],
        compiler_params=pltpu.CompilerParams(
            collective_id=0, has_side_effects=True, vmem_limit_bytes=60 * 1024 * 1024
        ),
    )(*flat)


def solution(mesh):
    in_specs = (
        P(("grp", "dp"), "ra"),
        P("ra"),
        P("ra", "cb"),
        P("ra", "cb"),
        P("cb", "ra"),
        P("cb"),
        P("cb"),
        P("ra"),
        P("ra"),
        P("ra", "cb"),
        P("ra", "cb"),
        P("cb", "ra"),
        P("cb"),
        P("cb"),
        P("ra"),
    )
    out_specs = P(("grp", "dp"), "ra")
    n, m = mesh.shape["ra"], mesh.shape["cb"]
    return jax.shard_map(
        functools.partial(per_device, n, m), mesh=mesh, in_specs=in_specs, out_specs=out_specs, check_vma=False
    )
```

```python
import functools

import jax
import jax.numpy as jnp
from jax import lax
from jax.experimental import pallas as pl
from jax.experimental.pallas import tpu as pltpu
from jax.sharding import PartitionSpec as P

EPS = 1e-06
MESH = pl.DeviceIdType.MESH
LANES = 128
LAG_SUM = 5
LAG_HID = 8


def kernel(dims, *refs):
    n, m, rows, width, units, total_width = dims
    (tokens, gain0, gate0, up0, down0, gs0, us0, ds0, gain1, gate1, up1, down1, gs1, us1, ds1) = refs[:15]
    out = refs[15]
    (values, scaled, gains, dscales, gscales, uscales, w_gu, w_down, own, sum_out, sum_in, cross_in, hid, acc,
     down_in, squares, inverse, small_sem, gate_sem, up_sem, down_sem, sum_ss, sum_rs, cross_rs, hid_ss, hid_rs,
     part_ss, part_rs, sq_ss, sq_rs) = refs[16:]
    gate, up, down = (gate0, gate1), (up0, up1), (down0, down1)
    bf16, f32 = jnp.bfloat16, jnp.float32

    z, x = lax.axis_index("ra"), lax.axis_index("cb")
    blocks = units // LANES
    half = n // 2
    owners = (half - 1, half)
    counts = (blocks - blocks // 2, blocks // 2)
    starts = (0, counts[0])
    left = z < half
    step = jnp.where(left, 1, -1)
    p = jnp.where(left, z, n - 1 - z)
    middle = (z == half - 1) | (z == half)
    first = jnp.where(left, counts[0], 0)
    n_far = jnp.where(left, counts[1], counts[0])
    depth = (half - 1, n - half - 1)
    slots = max(blocks + blocks // 2, blocks + LAG_SUM * max(depth) + LAG_HID)

    def copy_small():
        found = []
        for i, (src, dst) in enumerate((
            (tokens, values), (gain0, gains.at[0]), (gs0, gscales.at[0]), (us0, uscales.at[0]), (ds0, dscales.at[0]),
            (gain1, gains.at[1]), (gs1, gscales.at[1]), (us1, uscales.at[1]), (ds1, dscales.at[1]),
        )):
            found.append(pltpu.make_async_copy(src, dst, small_sem.at[i]))
        return found

    def columns(c):
        return pl.ds(pl.multiple_of(c * LANES, LANES), LANES)

    def gate_copy(l, c):
        return pltpu.make_async_copy(gate[l].at[:, columns(c)], w_gu.at[l, c, :, pl.ds(0, LANES)], gate_sem.at[l, c])

    def up_copy(l, c):
        return pltpu.make_async_copy(up[l].at[:, columns(c)], w_gu.at[l, c, :, pl.ds(LANES, LANES)], up_sem.at[l, c])

    def down_copy(l, c):
        return pltpu.make_async_copy(down[l].at[columns(c), :], w_down.at[l, c], down_sem.at[l, c])

    def sum_copy(l, c):
        return pltpu.make_async_remote_copy(
            src_ref=sum_out.at[l, c], dst_ref=sum_in.at[l, c], send_sem=sum_ss.at[l, c], recv_sem=sum_rs.at[l, c],
            device_id={"ra": z + step}, device_id_type=MESH)

    def cross_copy(l, c):
        return pltpu.make_async_remote_copy(
            src_ref=sum_out.at[l, c], dst_ref=cross_in.at[l, c], send_sem=sum_ss.at[l, c],
            recv_sem=cross_rs.at[l, c], device_id={"ra": z + step}, device_id_type=MESH)

    def hid_copy(l, c, o):
        return pltpu.make_async_remote_copy(
            src_ref=hid.at[l, c], dst_ref=hid.at[l, c], send_sem=hid_ss.at[l, o, c], recv_sem=hid_rs.at[l, c],
            device_id={"ra": lax.rem(z + o, n)}, device_id_type=MESH)

    def part_copy(l, o, sender):
        return pltpu.make_async_remote_copy(
            src_ref=down_in.at[l, sender], dst_ref=down_in.at[l, sender], send_sem=part_ss.at[l, o],
            recv_sem=part_rs.at[l, sender], device_id={"cb": lax.rem(x + o, m)}, device_id_type=MESH)

    def sq_copy(l, end, sender):
        return pltpu.make_async_remote_copy(
            src_ref=squares.at[l, sender], dst_ref=squares.at[l, sender], send_sem=sq_ss.at[l, end],
            recv_sem=sq_rs.at[l, sender], device_id={"ra": owners[end]}, device_id_type=MESH)

    def stream(j):
        return lax.rem(first + j, blocks)

    small = copy_small()
    for copy in small:
        copy.start()

    def start_first(i, carry):
        c = stream(i)
        gate_copy(0, c).start()
        up_copy(0, c).start()
        return carry

    lax.fori_loop(0, blocks, start_first, 0)

    barrier = pltpu.get_barrier_semaphore()
    for o in range(1, n):
        pl.semaphore_signal(barrier, inc=1, device_id={"ra": lax.rem(z + o, n)}, device_id_type=MESH)
    for o in range(1, m):
        pl.semaphore_signal(barrier, inc=1, device_id={"cb": lax.rem(x + o, m)}, device_id_type=MESH)
    for copy in small:
        copy.wait()

    for l in range(2):
        floats = values[...].astype(f32)
        scaled[...] = (floats * gains[l]).astype(bf16)
        squares[l, z] = lax.dot_general(
            jnp.ones((8, width), f32), floats * floats, (((1,), (1,)), ((), ())),
            precision=lax.Precision.HIGHEST, preferred_element_type=f32)
        acc[...] = jnp.zeros_like(acc)
        if l == 0:
            pl.semaphore_wait(barrier, n + m - 2)
        for end in range(2):
            @pl.when(z != owners[end])
            def _():
                sq_copy(l, end, z).start()

        def use_hidden(c, block):
            down_copy(l, c).wait()
            acc[...] += jnp.dot(block, w_down[l, c].astype(bf16), preferred_element_type=f32)

        def slot(s, carry):
            if l == 0:
                @pl.when(s < blocks)
                def _():
                    down_copy(0, stream(s)).start()

                later = s - blocks // 2

                @pl.when((later >= 0) & (later < blocks))
                def _():
                    c = stream(later)
                    gate_copy(1, c).start()
                    up_copy(1, c).start()
                    down_copy(1, c).start()

            @pl.when(s < blocks)
            def _():
                c = stream(s)
                gate_copy(l, c).wait()
                up_copy(l, c).wait()
                own[c] = jnp.dot(scaled[...], w_gu[l, c].astype(bf16), preferred_element_type=f32)

            k = s - LAG_SUM * p
            c = stream(jnp.clip(k, 0, blocks - 1))
            turn = (k >= 0) & (k < blocks)
            mine = middle & (k >= n_far)

            @pl.when(turn & jnp.logical_not(mine))
            def _():
                @pl.when(p == 0)
                def _():
                    sum_out[l, c] = own[c].astype(bf16)

                @pl.when(p > 0)
                def _():
                    sum_copy(l, c).wait_recv()
                    sum_out[l, c] = (own[c] + sum_in[l, c].astype(f32)).astype(bf16)

                @pl.when(middle)
                def _():
                    cross_copy(l, c).start()

                @pl.when(jnp.logical_not(middle))
                def _():
                    sum_copy(l, c).start()

            @pl.when(turn & mine)
            def _():
                @pl.when(k == n_far)
                def _():
                    for o in range(1, n):
                        sq_copy(l, 0, lax.rem(z + o, n)).wait_recv()
                    every = squares[l].reshape(8 * n, rows)
                    total = lax.dot_general(
                        every, jnp.full((8 * n, LANES), 0.125, f32), (((0,), (0,)), ((), ())),
                        precision=lax.Precision.HIGHEST, preferred_element_type=f32)
                    inverse[...] = lax.rsqrt(total / total_width + EPS)

                @pl.when(p > 0)
                def _():
                    sum_copy(l, c).wait_recv()
                    own[c] += sum_in[l, c].astype(f32)

                cross_copy(l, c).wait_recv()
                both = own[c] + cross_in[l, c].astype(f32)
                inv = inverse[...]
                g = both[:, :LANES] * gscales[l, pl.ds(c, 1), :] * inv
                u = both[:, LANES:] * uscales[l, pl.ds(c, 1), :] * inv
                block = (g / (1.0 + jnp.exp(-g)) * u).astype(bf16)
                hid[l, c] = block
                for o in range(1, n):
                    hid_copy(l, c, o).start()
                use_hidden(c, block)

            for d in range(2):
                k2 = s - counts[1 - d] - LAG_SUM * depth[d] - LAG_HID

                @pl.when((k2 >= 0) & (k2 < counts[d]) & (z != owners[d]))
                def _():
                    c2 = starts[d] + k2
                    hid_copy(l, c2, 1).wait_recv()
                    use_hidden(c2, hid[l, c2])
            return carry

        lax.fori_loop(0, slots, slot, 0)

        down_in[l, x] = acc[...].astype(bf16)
        for o in range(1, m):
            part_copy(l, o, x).start()
        for o in range(1, m):
            part_copy(l, o, lax.rem(x + o, m)).wait_recv()
        total = down_in[l, 0].astype(f32)
        for o in range(1, m):
            total = total + down_in[l, o].astype(f32)
        result = (0.3 * values[...].astype(f32) + 0.5 * total * dscales[l]).astype(bf16)
        if l == 0:
            values[...] = result
        else:
            out[...] = result

    for l in range(2):
        for o in range(1, m):
            part_copy(l, o, x).wait_send()
        for end in range(2):
            @pl.when(z != owners[end])
            def _():
                sq_copy(l, end, z).wait_send()
        def sent_sum(k, carry):
            sum_copy(l, stream(k)).wait_send()
            return carry

        lax.fori_loop(0, jnp.where(middle, n_far, blocks), sent_sum, 0)

        @pl.when(middle)
        def _():
            def sent_hid(k, carry):
                for o in range(1, n):
                    hid_copy(l, stream(n_far + k), o).wait_send()
                return carry
            lax.fori_loop(0, blocks - n_far, sent_hid, 0)


def per_device(n, m, *args):
    tokens = args[0]
    rows, width = tokens.shape
    units = args[2].shape[1]
    blocks = units // LANES
    bf16, f32 = jnp.bfloat16, jnp.float32
    flat = [a if a.ndim > 1 else a.reshape(1, width) if i in (1, 7, 8, 14) else a.reshape(blocks, LANES) for i, a in enumerate(args)]
    dma = pltpu.SemaphoreType.DMA
    return pl.pallas_call(
        functools.partial(kernel, (n, m, rows, width, units, n * width)),
        out_shape=jax.ShapeDtypeStruct((rows, width), bf16),
        in_specs=[pl.BlockSpec(memory_space=pl.ANY)] * len(flat),
        out_specs=pl.BlockSpec(memory_space=pltpu.VMEM),
        scratch_shapes=[
            pltpu.VMEM((rows, width), bf16),
            pltpu.VMEM((rows, width), bf16),
            pltpu.VMEM((2, 1, width), f32),
            pltpu.VMEM((2, 1, width), f32),
            pltpu.VMEM((2, blocks, LANES), f32),
            pltpu.VMEM((2, blocks, LANES), f32),
            pltpu.VMEM((2, blocks, width, 2 * LANES), f32),
            pltpu.VMEM((2, blocks, LANES, width), f32),
            pltpu.VMEM((blocks, rows, 2 * LANES), f32),
            pltpu.VMEM((2, blocks, rows, 2 * LANES), bf16),
            pltpu.VMEM((2, blocks, rows, 2 * LANES), bf16),
            pltpu.VMEM((2, blocks, rows, 2 * LANES), bf16),
            pltpu.VMEM((2, blocks, rows, LANES), bf16),
            pltpu.VMEM((rows, width), f32),
            pltpu.VMEM((2, m, rows, width), bf16),
            pltpu.VMEM((2, n, 8, rows), f32),
            pltpu.VMEM((rows, LANES), f32),
            dma((9,)),
            dma((2, blocks)),
            dma((2, blocks)),
            dma((2, blocks)),
            dma((2, blocks)),
            dma((2, blocks)),
            dma((2, blocks)),
            dma((2, n, blocks)),
            dma((2, blocks)),
            dma((2, m)),
            dma((2, m)),
            dma((2, 2)),
            dma((2, n)),
        ],
        compiler_params=pltpu.CompilerParams(
            collective_id=0, has_side_effects=True, vmem_limit_bytes=60 * 1024 * 1024
        ),
    )(*flat)


def solution(mesh):
    in_specs = (
        P(("grp", "dp"), "ra"),
        P("ra"),
        P("ra", "cb"),
        P("ra", "cb"),
        P("cb", "ra"),
        P("cb"),
        P("cb"),
        P("ra"),
        P("ra"),
        P("ra", "cb"),
        P("ra", "cb"),
        P("cb", "ra"),
        P("cb"),
        P("cb"),
        P("ra"),
    )
    out_specs = P(("grp", "dp"), "ra")
    n, m = mesh.shape["ra"], mesh.shape["cb"]
    return jax.shard_map(
        functools.partial(per_device, n, m), mesh=mesh, in_specs=in_specs, out_specs=out_specs, check_vma=False
    )
```
